32 devices in a mesh: sp: 4 (over z), fs: 4 (over y, x), tp: 2 (over core).
Axes of the slice: x: 2, y: 2, z: 4, core: 2. Of those that a mesh axis runs over, the one named last changes fastest.
Arguments:
- hidden_in: bfloat16 [4, 1024, 2048], P('fs', 'sp', 'tp'), may hold values from -6 to 6
- sb_query_w: bfloat16 [2048, 1024], P('fs', 'tp'), may hold values from -0.21875 to 0.21875
- sb_key_w: bfloat16 [2048, 1024], P('fs', 'tp'), may hold values from -0.21875 to 0.21875
- sb_value_w: bfloat16 [2048, 1024], P('fs', 'tp'), may hold values from -0.125 to 0.125
- sb_offset: float32 [16], P('tp'), may hold values from -16 to -6
- delta_query_w: bfloat16 [2048, 1024], P('fs', 'tp'), may hold values from -0.125 to 0.125
- delta_key_w: bfloat16 [2048, 1024], P('fs', 'tp'), may hold values from -0.125 to 0.125
- delta_value_w: bfloat16 [2048, 1024], P('fs', 'tp'), may hold values from -0.125 to 0.125
- decay_w: bfloat16 [2048, 8], P(None, 'tp'), may hold values from -0.125 to 0.125
- write_w: bfloat16 [2048, 8], P(None, 'tp'), may hold values from -0.125 to 0.125
- write_bias: float32 [8], P('tp'), may hold values from -7 to 1.5
- decay_log_scale: float32 [8], P('tp'), may hold values from -14 to -3
- decay_shift: float32 [4, 8, 1024], P('fs', 'tp', 'sp'), may hold values from -3 to 0
- head_gain: float32 [128], replicated, may hold values from 0.1 to 1.9
- sb_out_w: bfloat16 [1024, 2048], P('tp'), may hold values from -0.125 to 0.125
- delta_out_w: bfloat16 [1024, 2048], P('tp'), may hold values from -0.125 to 0.125
Outputs:
- mixed_out: bfloat16 [4, 1024, 2048], P('fs', ('sp', 'tp'))
The draws below stay inside these ranges and needn't reach their ends.
All inputs are finite; a program needn't handle non-finite values.
Results may differ from the reference program's by a relative error of at most 0.015.
Values may be sent and summed in bfloat16 or wider, within the bound.
A program may use at most 128 MiB of HBM per device.

```python
import jax
import jax.numpy as jnp
from jax import lax

D = 2048
SB_HEADS = 16
SB_DIM = 64
GDN_HEADS = 8
GDN_DIM = 128
BLOCK = 64
TOK_DEV = 256
LEN = 1024
SEQS = 4
N_TP = 2


def head_kinds(key, fast_share):
    return jax.random.uniform(jax.random.fold_in(key, 71), (GDN_HEADS,), jnp.float32) < fast_share


def draw_sb_offset(key, part):
    reach_term = jax.random.uniform(key, (SB_HEADS,), jnp.float32, -1.0, 2.5)
    return reach_term - jnp.log(jnp.float32(LEN)) - 4.5


def draw_write_bias(key, part):
    fast_share = 0.5
    chosen = head_kinds(key, fast_share)
    strong_term = jax.random.uniform(jax.random.fold_in(key, 5), (GDN_HEADS,), jnp.float32, -1.0, 1.5)
    faint_summand = jax.random.uniform(jax.random.fold_in(key, 6), (GDN_HEADS,), jnp.float32, -7.0, -5.5)
    return jnp.where(chosen, strong_term, faint_summand)


def draw_decay_log_scale(key, part):
    split_keys = jax.random.split(key, 3)
    fast_share = 0.5
    chosen = head_kinds(key, fast_share)
    fast_rate = jax.random.uniform(split_keys[1], (GDN_HEADS,), jnp.float32, 0.015, 0.04)
    slow_rate = jax.random.uniform(split_keys[2], (GDN_HEADS,), jnp.float32, 2e-06, 8e-06)
    return jnp.log(jnp.where(chosen, fast_rate, slow_rate))


def draw_decay_shift(key, part):
    split_keys = jax.random.split(key, 3)
    blocks_count = LEN // TOK_DEV
    minimal_level = 0.15
    highest = 1.2
    rates = jnp.exp(jax.random.uniform(split_keys[0], (SEQS, GDN_HEADS, blocks_count), jnp.float32, jnp.log(minimal_level), jnp.log(highest)))
    unweighted_result = jnp.repeat(rates, TOK_DEV, axis=2) * (-1.0 / LEN)
    destination_indices = jax.random.randint(split_keys[1], (SEQS, GDN_HEADS, 3), 0, LEN)
    forgetting_amounts = jnp.log(jax.random.uniform(split_keys[2], (SEQS, GDN_HEADS, 3), jnp.float32, 0.5, 0.8))
    cell_locations = jnp.arange(LEN, dtype=jnp.int32)
    storing_pulses = jnp.sum(jnp.where(cell_locations[None, None, None, :] == destination_indices[..., None], forgetting_amounts[..., None], 0.0), axis=2)
    return unweighted_result + storing_pulses


def shard_levels(own_key, dims, pieces, smallest, top_value):
    gain, own = 1.0, jax.random.fold_in(own_key, 6)
    for axis_at, blocks in pieces:
        heights = jnp.exp(jax.random.uniform(jax.random.fold_in(own, axis_at), (blocks,), jnp.float32, smallest / len(pieces), top_value / len(pieces)))
        gain = gain * jnp.repeat(heights, dims[axis_at] // blocks).reshape([-1 if axis == axis_at else 1 for axis in range(len(dims))])
    return gain


def gaussian(own_key, dims, scale, reach, shards=(), kind=jnp.bfloat16):
    drawn = jax.random.normal(own_key, dims, jnp.float32) * scale
    if len(shards) > 0:
        drawn = shard_levels(own_key, dims, shards, -0.22, 0.18) * drawn
    return jnp.clip(drawn, min=-reach, max=reach).astype(kind)


def setup_inputs(seed: int = 0) -> dict:
    streams_of = jax.random.split(jax.random.key(seed), 17)
    hidden_in = gaussian(streams_of[0], (SEQS, LEN, D), 1.0, 6.0, ((0, 4), (1, 4), (2, 2)))
    sb_query_w = gaussian(streams_of[1], (D, SB_HEADS * SB_DIM), (D // 3) ** -0.5, 0.21875, ((0, 4), (1, 2)))
    sb_key_w = gaussian(streams_of[2], (D, SB_HEADS * SB_DIM), (D // 3) ** -0.5, 0.21875, ((0, 4), (1, 2)))
    sb_value_w = gaussian(streams_of[3], (D, SB_HEADS * SB_DIM), D ** -0.5, 0.125, ((0, 4), (1, 2)))
    sb_offset = draw_sb_offset(jax.random.fold_in(streams_of[16], 71), 0)
    delta_query_w = gaussian(streams_of[5], (D, GDN_HEADS * GDN_DIM), D ** -0.5, 0.125, ((0, 4), (1, 2)))
    delta_key_w = gaussian(streams_of[6], (D, GDN_HEADS * GDN_DIM), D ** -0.5, 0.125, ((0, 4), (1, 2)))
    delta_value_w = gaussian(streams_of[7], (D, GDN_HEADS * GDN_DIM), D ** -0.5, 0.125, ((0, 4), (1, 2)))
    decay_w = gaussian(streams_of[8], (D, GDN_HEADS), D ** -0.5, 0.125, ((1, 2),))
    write_w = gaussian(streams_of[9], (D, GDN_HEADS), D ** -0.5, 0.125, ((1, 2),))
    write_bias = draw_write_bias(jax.random.fold_in(streams_of[16], 71), 0)
    decay_log_scale = draw_decay_log_scale(jax.random.fold_in(streams_of[16], 71), 0)
    decay_shift = draw_decay_shift(jax.random.fold_in(streams_of[16], 71), 0)
    head_gain = jnp.clip(1.0 + 0.18 * jax.random.normal(streams_of[13], (GDN_DIM,), jnp.float32), 0.1, 1.9)
    sb_out_w = gaussian(streams_of[14], (SB_HEADS * SB_DIM, D), (SB_HEADS * SB_DIM + GDN_HEADS * GDN_DIM) ** -0.5, 0.125, ((0, 2),))
    delta_out_w = gaussian(streams_of[15], (GDN_HEADS * GDN_DIM, D), (SB_HEADS * SB_DIM + GDN_HEADS * GDN_DIM) ** -0.5, 0.125, ((0, 2),))
    return dict(hidden_in=hidden_in, sb_query_w=sb_query_w, sb_key_w=sb_key_w, sb_value_w=sb_value_w, sb_offset=sb_offset, delta_query_w=delta_query_w, delta_key_w=delta_key_w, delta_value_w=delta_value_w, decay_w=decay_w, write_w=write_w, write_bias=write_bias, decay_log_scale=decay_log_scale, decay_shift=decay_shift, head_gain=head_gain, sb_out_w=sb_out_w, delta_out_w=delta_out_w)


EXACT_MATMUL = lax.Precision.HIGHEST
NORM_EPS = 1e-06

def unit_lower_inverse(strict_part):
    order_size = strict_part.shape[-1]
    powered = strict_part
    inverse = jnp.eye(order_size, dtype=strict_part.dtype) - strict_part
    for repeat_number in range(max(1, (order_size - 1).bit_length()) - 1):
        powered = jnp.einsum('...ij,...jk->...ik', powered, powered, precision=EXACT_MATMUL)
        inverse = inverse + jnp.einsum('...ij,...jk->...ik', inverse, powered, precision=EXACT_MATMUL)
    return inverse

def to_blocks(row_data, block_span):
    blocks_count = row_data.shape[0] // block_span
    shaped = row_data.reshape((blocks_count, block_span) + row_data.shape[1:])
    return jnp.swapaxes(shaped, 1, 2)

def from_blocks(blocked):
    swapped = jnp.swapaxes(blocked, 1, 2)
    return swapped.reshape((-1,) + swapped.shape[2:])

def unit_rows(vectors):
    return vectors * lax.rsqrt(lax.optimization_barrier(jnp.sum(vectors * vectors, axis=-1, keepdims=True)) + NORM_EPS)

def delta_inputs(query_proj, key_proj, value_proj, decay_pre, write_pre, write_bias, decay_log_scale, shift_rows, head_count, head_size):
    query_act = jax.nn.silu(query_proj.astype(jnp.float32)).reshape(-1, head_count, head_size)
    key_act = jax.nn.silu(key_proj.astype(jnp.float32)).reshape(-1, head_count, head_size)
    value_rows = jax.nn.silu(value_proj.astype(jnp.float32)).reshape(-1, head_count, head_size)
    queries = unit_rows(query_act) * head_size ** (-0.5)
    key_rows = unit_rows(key_act)
    log_decay = -jnp.exp(decay_log_scale) * jax.nn.softplus(decay_pre) + shift_rows
    strength = jax.nn.sigmoid(write_pre + write_bias)
    return (queries, key_rows, value_rows, log_decay, strength)

def delta_prepare(queries, key_rows, value_rows, log_decay, strength):
    block_span = queries.shape[2]
    cumulative = jnp.cumsum(log_decay, axis=-1)
    row_place = lax.broadcasted_iota(jnp.int32, (block_span, block_span), 0)
    col_place = lax.broadcasted_iota(jnp.int32, (block_span, block_span), 1)
    inclusive = col_place <= row_place
    strictly = col_place < row_place
    spread = cumulative[..., :, None] - cumulative[..., None, :]
    decay_table = jnp.where(inclusive, jnp.exp(jnp.where(inclusive, spread, 0.0)), 0.0)
    keys_beta = key_rows * strength[..., None]
    lower_part = jnp.where(strictly, jnp.einsum('nhik,nhjk->nhij', keys_beta, key_rows, precision=EXACT_MATMUL) * decay_table, 0.0)
    inverse = unit_lower_inverse(lower_part)
    growth = jnp.exp(cumulative)
    state_updates = jnp.einsum('nhij,nhjv->nhiv', inverse, value_rows * strength[..., None], precision=EXACT_MATMUL)
    erase_term = jnp.einsum('nhij,nhjk->nhik', inverse, keys_beta * growth[..., None], precision=EXACT_MATMUL)
    inside_block = jnp.einsum('nhik,nhjk->nhij', queries, key_rows, precision=EXACT_MATMUL) * decay_table
    boosted_query = queries * growth[..., None]
    damped_keys = key_rows * jnp.exp(cumulative[..., -1:] - cumulative)[..., None]
    decay_per_block = jnp.exp(cumulative[..., -1])
    return (state_updates, erase_term, inside_block, boosted_query, damped_keys, decay_per_block)

def delta_step(memory_state, inputs):
    state_updates, erase_term, inside_block, boosted_query, damped_keys, decay_per_block = inputs
    fixed_values = state_updates - jnp.einsum('mzq,mqc->mzc', erase_term, memory_state, precision=EXACT_MATMUL)
    produced_rows = jnp.einsum('mzq,mqc->mzc', boosted_query, memory_state, precision=EXACT_MATMUL) + jnp.einsum('efq,eqn->efn', inside_block, fixed_values, precision=EXACT_MATMUL)
    memory_state = memory_state * decay_per_block[:, None, None] + jnp.einsum('wam,waz->wmz', damped_keys, fixed_values, precision=EXACT_MATMUL)
    return (memory_state, produced_rows)

def stick_block(queries, key_rows, value_rows, query_place, key_place, offsets):
    scale_factor = queries.shape[-1] ** (-0.5)
    scores = jnp.einsum('qhd,khd->hqk', queries.astype(jnp.float32), key_rows.astype(jnp.float32)) * scale_factor + offsets[:, None, None]
    visible = key_place[None, :] < query_place[:, None]
    skipped = jnp.where(visible, jax.nn.log_sigmoid(-scores), 0.0)
    beyond = lax.cumsum(skipped, axis=2, reverse=True) - skipped
    weights = jnp.where(visible, jnp.exp(jax.nn.log_sigmoid(scores) + beyond), 0.0).astype(jnp.bfloat16)
    weights = lax.optimization_barrier(weights).astype(jnp.float32)
    partial_value = jnp.einsum('hqk,khd->qhd', weights, value_rows.astype(jnp.float32))
    return (partial_value, lax.optimization_barrier(jnp.sum(skipped, axis=2)).T)

def stick_combine(partials, totals):
    beyond = jnp.cumsum(totals[::-1], axis=0)[::-1] - totals
    return lax.optimization_barrier(jnp.sum(partials * jnp.exp(beyond)[..., None], axis=0))

def stick_sequence(queries, key_rows, value_rows, offsets):
    blocks_count = LEN // TOK_DEV
    query_blocks = queries.reshape((blocks_count, TOK_DEV) + queries.shape[1:])
    key_blocks = key_rows.reshape((blocks_count, TOK_DEV) + key_rows.shape[1:])
    value_blocks = value_rows.reshape((blocks_count, TOK_DEV) + value_rows.shape[1:])
    cell_locations = jnp.arange(LEN, dtype=jnp.int32).reshape(blocks_count, TOK_DEV)
    head_count = queries.shape[1]
    head_size = value_rows.shape[2]

    def per_query(query_index):

        def per_key(key_index):

            def active(unused_arg):
                return stick_block(query_blocks[query_index], key_blocks[key_index], value_blocks[key_index], cell_locations[query_index], cell_locations[key_index], offsets)

            def inactive(unused_arg):
                return (jnp.zeros((TOK_DEV, head_count, head_size), jnp.float32), jnp.zeros((TOK_DEV, head_count), jnp.float32))
            return lax.cond(key_index <= query_index, active, inactive, 0)
        partials, totals = lax.map(per_key, jnp.arange(blocks_count, dtype=jnp.int32))
        return stick_combine(partials, totals)
    gathered = lax.map(per_query, jnp.arange(blocks_count, dtype=jnp.int32))
    return gathered.reshape(LEN, head_count, head_size)

def reference(hidden_in, sb_query_w, sb_key_w, sb_value_w, sb_offset, delta_query_w, delta_key_w, delta_value_w, decay_w, write_w, write_bias, decay_log_scale, decay_shift, head_gain, sb_out_w, delta_out_w):

    def one_sequence(inputs):
        sequence_rows, shift_rows = inputs

        def project(weight):
            return jnp.dot(sequence_rows, weight, preferred_element_type=jnp.float32).astype(jnp.bfloat16)
        sb_query = project(sb_query_w).reshape(LEN, SB_HEADS, SB_DIM)
        sb_keys = project(sb_key_w).reshape(LEN, SB_HEADS, SB_DIM)
        sb_values = project(sb_value_w).reshape(LEN, SB_HEADS, SB_DIM)
        sb_mixed = stick_sequence(sb_query, sb_keys, sb_values, sb_offset).astype(jnp.bfloat16).reshape(LEN, SB_HEADS * SB_DIM)
        decay_pre = jnp.dot(sequence_rows, decay_w, preferred_element_type=jnp.float32)
        write_pre = jnp.dot(sequence_rows, write_w, preferred_element_type=jnp.float32)
        queries, key_rows, value_rows, log_decay, strength = delta_inputs(project(delta_query_w), project(delta_key_w), project(delta_value_w), decay_pre, write_pre, write_bias, decay_log_scale, shift_rows.T, GDN_HEADS, GDN_DIM)
        prepared = delta_prepare(to_blocks(queries, BLOCK), to_blocks(key_rows, BLOCK), to_blocks(value_rows, BLOCK), to_blocks(log_decay, BLOCK), to_blocks(strength, BLOCK))
        initial = jnp.zeros((GDN_HEADS, GDN_DIM, GDN_DIM), jnp.float32)
        unused_memory, produced_rows = lax.scan(delta_step, initial, prepared)
        produced_rows = from_blocks(produced_rows)
        normed = produced_rows * lax.rsqrt(lax.optimization_barrier(jnp.mean(produced_rows * produced_rows, axis=-1, keepdims=True)) + NORM_EPS) * head_gain
        delta_mixed = normed.astype(jnp.bfloat16).reshape(LEN, GDN_HEADS * GDN_DIM)
        sb_group = SB_HEADS * SB_DIM // N_TP
        delta_group = GDN_HEADS * GDN_DIM // N_TP
        accumulated = jnp.zeros((LEN, D), jnp.float32)
        for group_number in range(N_TP):
            sb_cols = slice(group_number * sb_group, (group_number + 1) * sb_group)
            delta_cols = slice(group_number * delta_group, (group_number + 1) * delta_group)
            term = jnp.dot(sb_mixed[:, sb_cols], sb_out_w[sb_cols], preferred_element_type=jnp.float32) + jnp.dot(delta_mixed[:, delta_cols], delta_out_w[delta_cols], preferred_element_type=jnp.float32)
            rounded = lax.optimization_barrier(term.astype(jnp.bfloat16))
            accumulated = accumulated + rounded.astype(jnp.float32)
        return accumulated.astype(jnp.bfloat16)
    return lax.map(one_sequence, (hidden_in, decay_shift))
```

```python
import jax
import jax.numpy as jnp
from jax import lax
from jax.experimental import pallas as pl
from jax.experimental.pallas import tpu as pltpu
from jax.sharding import PartitionSpec as P

MESH = pl.DeviceIdType.MESH

SB_DIM = 64
GDN_DIM = 128
BLOCK = 64


EXACT_MATMUL = lax.Precision.HIGHEST
NORM_EPS = 1e-06


def carried_in(value, axis, combine, identity):
    devices, index = (lax.axis_size(axis), lax.axis_index(axis))
    everything = jax.tree.map(
        lambda part, kind: lax.all_gather(part.astype(kind), axis),
        value,
        (jnp.bfloat16, jnp.bfloat16),
    )
    start = jax.tree.map(
        lambda part, zero: jnp.broadcast_to(jnp.asarray(zero, part.dtype), part.shape),
        value,
        identity,
    )

    def lap(k, before):
        reached = k < index
        new = combine(
            before, jax.tree.map(lambda part, own: part[k].astype(own.dtype), everything, value)
        )
        return jax.tree.map(lambda a, b: jnp.where(reached, a, b), new, before)

    return lax.fori_loop(0, devices, lap, start)


def unit_lower_inverse(strict_part):
    order_size = strict_part.shape[-1]
    powered = strict_part
    inverse = jnp.eye(order_size, dtype=strict_part.dtype) - strict_part
    for repeat_number in range(max(1, (order_size - 1).bit_length()) - 1):
        powered = jnp.einsum("...ij,...jk->...ik", powered, powered, precision=EXACT_MATMUL)
        inverse = inverse + jnp.einsum(
            "...ij,...jk->...ik", inverse, powered, precision=EXACT_MATMUL
        )
    return inverse


def to_blocks(row_data, block_span):
    blocks_count = row_data.shape[0] // block_span
    shaped = row_data.reshape((blocks_count, block_span) + row_data.shape[1:])
    return jnp.swapaxes(shaped, 1, 2)


def from_blocks(blocked):
    swapped = jnp.swapaxes(blocked, 1, 2)
    return swapped.reshape((-1,) + swapped.shape[2:])


def unit_rows(vectors):
    return vectors * lax.rsqrt(jnp.sum(vectors * vectors, axis=-1, keepdims=True) + NORM_EPS)


def delta_inputs(
    query_proj,
    key_proj,
    value_proj,
    decay_pre,
    write_pre,
    write_bias,
    decay_log_scale,
    shift_rows,
    head_count,
    head_size,
):
    query_act = jax.nn.silu(query_proj.astype(jnp.float32)).reshape(-1, head_count, head_size)
    key_act = jax.nn.silu(key_proj.astype(jnp.float32)).reshape(-1, head_count, head_size)
    value_rows = jax.nn.silu(value_proj.astype(jnp.float32)).reshape(-1, head_count, head_size)
    queries = unit_rows(query_act) * head_size ** (-0.5)
    key_rows = unit_rows(key_act)
    log_decay = -jnp.exp(decay_log_scale) * jax.nn.softplus(decay_pre) + shift_rows
    strength = jax.nn.sigmoid(write_pre + write_bias)
    return (queries, key_rows, value_rows, log_decay, strength)


def delta_prepare(queries, key_rows, value_rows, log_decay, strength):
    block_span = queries.shape[2]
    cumulative = jnp.cumsum(log_decay, axis=-1)
    row_place = lax.broadcasted_iota(jnp.int32, (block_span, block_span), 0)
    col_place = lax.broadcasted_iota(jnp.int32, (block_span, block_span), 1)
    inclusive = col_place <= row_place
    strictly = col_place < row_place
    spread = cumulative[..., :, None] - cumulative[..., None, :]
    decay_table = jnp.where(inclusive, jnp.exp(jnp.where(inclusive, spread, 0.0)), 0.0)
    keys_beta = key_rows * strength[..., None]
    lower_part = jnp.where(
        strictly,
        jnp.einsum("nhik,nhjk->nhij", keys_beta, key_rows, precision=EXACT_MATMUL) * decay_table,
        0.0,
    )
    inverse = unit_lower_inverse(lower_part)
    growth = jnp.exp(cumulative)
    state_updates = jnp.einsum(
        "nhij,nhjv->nhiv", inverse, value_rows * strength[..., None], precision=EXACT_MATMUL
    )
    erase_term = jnp.einsum(
        "nhij,nhjk->nhik", inverse, keys_beta * growth[..., None], precision=EXACT_MATMUL
    )
    inside_block = (
        jnp.einsum("nhik,nhjk->nhij", queries, key_rows, precision=EXACT_MATMUL) * decay_table
    )
    boosted_query = queries * growth[..., None]
    damped_keys = key_rows * jnp.exp(cumulative[..., -1:] - cumulative)[..., None]
    decay_per_block = jnp.exp(cumulative[..., -1])
    return (state_updates, erase_term, inside_block, boosted_query, damped_keys, decay_per_block)


def delta_step(memory_state, inputs):
    state_updates, erase_term, inside_block, boosted_query, damped_keys, decay_per_block = inputs
    fixed_values = state_updates - jnp.einsum(
        "mzq,mqc->mzc", erase_term, memory_state, precision=EXACT_MATMUL
    )
    produced_rows = jnp.einsum(
        "mzq,mqc->mzc", boosted_query, memory_state, precision=EXACT_MATMUL
    ) + jnp.einsum("efq,eqn->efn", inside_block, fixed_values, precision=EXACT_MATMUL)
    memory_state = memory_state * decay_per_block[:, None, None] + jnp.einsum(
        "wam,waz->wmz", damped_keys, fixed_values, precision=EXACT_MATMUL
    )
    return (memory_state, produced_rows)


def transition_step(carried, inputs):
    memory_state, transfer = carried
    state_updates, erase_term, inside_block, boosted_query, damped_keys, decay_per_block = inputs
    fixed_values = state_updates - jnp.einsum(
        "mzq,mqc->mzc", erase_term, memory_state, precision=EXACT_MATMUL
    )
    coupling = jnp.einsum("hik,hil->hkl", damped_keys, erase_term, precision=EXACT_MATMUL)
    memory_state = memory_state * decay_per_block[:, None, None] + jnp.einsum(
        "wam,waz->wmz", damped_keys, fixed_values, precision=EXACT_MATMUL
    )
    transfer = transfer * decay_per_block[:, None, None] - jnp.einsum(
        "hkl,hlm->hkm", coupling, transfer, precision=EXACT_MATMUL
    )
    return ((memory_state, transfer), None)


def compose(prior_blocks, following_blocks):
    joined_map = jnp.einsum(
        "hkl,hlm->hkm", following_blocks[0], prior_blocks[0], precision=EXACT_MATMUL
    )
    joined_state = (
        jnp.einsum("djo,dog->djg", following_blocks[0], prior_blocks[1], precision=EXACT_MATMUL)
        + following_blocks[1]
    )
    return (joined_map, joined_state)


def stick_block(queries, key_rows, value_rows, query_place, key_place, offsets):
    scale_factor = queries.shape[-1] ** (-0.5)
    scores = (
        jnp.einsum("qhd,khd->hqk", queries, key_rows, preferred_element_type=jnp.float32)
        * scale_factor
        + offsets[:, None, None]
    )
    visible = key_place[None, :] < query_place[:, None]
    skipped = jnp.where(visible, jax.nn.log_sigmoid(-scores), 0.0)
    beyond = lax.cumsum(skipped, axis=2, reverse=True) - skipped
    weights = jnp.where(visible, jnp.exp(jax.nn.log_sigmoid(scores) + beyond), 0.0).astype(
        jnp.bfloat16
    )
    partial_value = jnp.einsum(
        "hqk,khd->qhd", weights, value_rows, preferred_element_type=jnp.float32
    )
    return (partial_value, jnp.sum(skipped, axis=2).T)


def stick_combine(partials, totals):
    beyond = jnp.cumsum(totals[::-1], axis=0)[::-1] - totals
    return jnp.sum(partials * jnp.exp(beyond)[..., None], axis=0)


def on_device_split(
    hidden_in,
    sb_query_w,
    sb_key_w,
    sb_value_w,
    sb_offset,
    delta_query_w,
    delta_key_w,
    delta_value_w,
    decay_w,
    write_w,
    write_bias,
    decay_log_scale,
    decay_shift,
    head_gain,
    sb_out_w,
    delta_out_w,
):
    token_rows = hidden_in.shape[1]
    local_in = hidden_in.reshape(token_rows, hidden_in.shape[2])
    gathered = (
        lax.all_gather(sb_query_w, "fs", axis=0, tiled=True),
        lax.all_gather(sb_key_w, "fs", axis=0, tiled=True),
        lax.all_gather(sb_value_w, "fs", axis=0, tiled=True),
        lax.all_gather(delta_query_w, "fs", axis=0, tiled=True),
        lax.all_gather(delta_key_w, "fs", axis=0, tiled=True),
        lax.all_gather(delta_value_w, "fs", axis=0, tiled=True),
    )
    in_weights = tuple(gathered) + (decay_w, write_w)
    portion = lax.all_gather(local_in, "tp", axis=1, tiled=True)
    projected = tuple(
        (jnp.dot(portion, weight, preferred_element_type=jnp.float32) for weight in in_weights)
    )
    sb_heads = sb_offset.shape[0]
    delta_heads = decay_log_scale.shape[0]
    sb_query = projected[0].astype(jnp.bfloat16).reshape(token_rows, sb_heads, SB_DIM)
    sb_keys = projected[1].astype(jnp.bfloat16)
    sb_values = projected[2].astype(jnp.bfloat16)
    shift_rows = decay_shift.reshape(delta_heads, token_rows).T
    queries, key_rows, value_rows, log_decay, strength = delta_inputs(
        projected[3].astype(jnp.bfloat16),
        projected[4].astype(jnp.bfloat16),
        projected[5].astype(jnp.bfloat16),
        projected[6],
        projected[7],
        write_bias,
        decay_log_scale,
        shift_rows,
        delta_heads,
        GDN_DIM,
    )
    prepared = delta_prepare(
        to_blocks(queries, BLOCK),
        to_blocks(key_rows, BLOCK),
        to_blocks(value_rows, BLOCK),
        to_blocks(log_decay, BLOCK),
        to_blocks(strength, BLOCK),
    )
    identity_map = jnp.broadcast_to(
        jnp.eye(GDN_DIM, dtype=jnp.float32), (delta_heads, GDN_DIM, GDN_DIM)
    )
    empty_state = jnp.zeros((delta_heads, GDN_DIM, GDN_DIM), jnp.float32)
    (local_end, local_map), unused_out = lax.scan(
        transition_step, (empty_state, identity_map), prepared
    )
    own_first = lax.axis_index("sp") * token_rows
    query_place = own_first + lax.iota(jnp.int32, token_rows)
    sp_count = lax.axis_size("sp")
    slot_out = jnp.zeros((sp_count, token_rows, sb_heads, SB_DIM), jnp.float32)
    slot_total = jnp.zeros((sp_count, token_rows, sb_heads), jnp.float32)

    def absorb(slot_arrays, address_portion, value_part, shard_first):

        def active(current):
            partial_value, totals = stick_block(
                sb_query,
                address_portion.reshape(token_rows, sb_heads, SB_DIM),
                value_part.reshape(token_rows, sb_heads, SB_DIM),
                query_place,
                shard_first + lax.iota(jnp.int32, token_rows),
                sb_offset,
            )
            slot_index = shard_first // token_rows
            return (
                lax.dynamic_update_index_in_dim(current[0], partial_value, slot_index, 0),
                lax.dynamic_update_index_in_dim(current[1], totals, slot_index, 0),
            )

        def inactive(current):
            return current

        usable = jnp.logical_and(shard_first >= 0, shard_first <= own_first)
        return lax.cond(usable, active, inactive, slot_arrays)

    key_block = lax.all_gather(sb_keys, "sp", axis=0, tiled=True)
    value_block = lax.all_gather(sb_values, "sp", axis=0, tiled=True)

    def per_shard(shard_number, current):
        row_begin = shard_number * token_rows
        return absorb(
            current,
            lax.dynamic_slice_in_dim(key_block, row_begin, token_rows, 0),
            lax.dynamic_slice_in_dim(value_block, row_begin, token_rows, 0),
            row_begin,
        )

    slot_arrays = lax.fori_loop(
        0, key_block.shape[0] // token_rows, per_shard, (slot_out, slot_total)
    )
    unused_map, incoming = carried_in(
        (local_map, local_end), "sp", compose, (identity_map, empty_state)
    )
    sb_mixed = (
        stick_combine(slot_arrays[0], slot_arrays[1])
        .astype(jnp.bfloat16)
        .reshape(token_rows, sb_heads * SB_DIM)
    )
    unused_end, produced_rows = lax.scan(delta_step, incoming, prepared)
    produced_rows = from_blocks(produced_rows)
    normed = (
        produced_rows
        * lax.rsqrt(jnp.mean(produced_rows * produced_rows, axis=-1, keepdims=True) + NORM_EPS)
        * head_gain
    )
    delta_mixed = normed.astype(jnp.bfloat16).reshape(token_rows, delta_heads * GDN_DIM)
    result = lax.psum_scatter(
        (
            jnp.dot(sb_mixed, sb_out_w, preferred_element_type=jnp.float32)
            + jnp.dot(delta_mixed, delta_out_w, preferred_element_type=jnp.float32)
        ).astype(jnp.bfloat16),
        "tp",
        scatter_dimension=0,
        tiled=True,
    ).astype(jnp.float32)
    return result.astype(jnp.bfloat16).reshape(1, result.shape[0], result.shape[1])


def remote(src, dst, send, recv, axis, index):
    return pltpu.make_async_remote_copy(
        src_ref=src, dst_ref=dst, send_sem=send, recv_sem=recv,
        device_id={axis: index}, device_id_type=MESH,
    )


def greet(axes):
    barrier = pltpu.get_barrier_semaphore()
    count = 0
    for axis in axes:
        size, me = lax.axis_size(axis), lax.axis_index(axis)
        for k in range(1, size):
            pl.semaphore_signal(
                barrier, inc=1, device_id={axis: lax.rem(me + k, size)}, device_id_type=MESH
            )
            count += 1
    pl.semaphore_wait(barrier, count)


def project_kernel(
    x_ref, w0, w1, w2, w3, w4, w5, gates_ref, shift_ref,
    p_ref, pre_ref, shifts_ref,
    xs, ws, x_send, x_recv, f_send, f_recv, w_send, w_recv, s_send, s_recv, l_sem, lw_sem,
):
    weights = (w0, w1, w2, w3, w4, w5)
    sp, fs, tp = lax.axis_size("sp"), lax.axis_size("fs"), lax.axis_size("tp")
    z, f, t = lax.axis_index("sp"), lax.axis_index("fs"), lax.axis_index("tp")
    rows, half = x_ref.shape
    depth = w0.shape[0]
    cols = ws.shape[1] // len(weights)
    own_x = pltpu.make_async_copy(
        x_ref, xs.at[z, :, pl.ds(pl.multiple_of(t * half, half), half)], l_sem.at[0]
    )
    own_x.start()
    own_shift = pltpu.make_async_copy(shift_ref, shifts_ref.at[z], l_sem.at[1])
    own_shift.start()

    def w_src(i, who):
        return weights[i].at[:, pl.ds(pl.multiple_of(who * cols, cols), cols)]

    def w_dst(i):
        return ws.at[pl.ds(pl.multiple_of(f * depth, depth), depth), pl.ds(i * cols, cols)]

    own_w = [
        pltpu.make_async_copy(w_src(i, z), w_dst(i), lw_sem.at[i]) for i in range(len(weights))
    ]
    for c in own_w:
        c.start()
    greet(("sp", "fs", "tp"))
    slot = pl.ds(pl.multiple_of(t * half, half), half)
    w_copies, x_copies, s_copies, f_copies = [], [], [], []
    for k in range(1, sp):
        c = remote(
            x_ref, xs.at[z, :, slot], x_send.at[k], x_recv.at[k], "sp", lax.rem(z + k, sp)
        )
        c.start()
        x_copies.append(c)
    for k in range(1, fs):
        for i in range(len(weights)):
            c = remote(
                w_src(i, z), w_dst(i), w_send.at[k, i], w_recv.at[k, i],
                "fs", lax.rem(f + k, fs),
            )
            c.start()
            w_copies.append(c)
    for k in range(1, sp):
        c = remote(
            shift_ref, shifts_ref.at[z], s_send.at[k], s_recv.at[k], "sp", lax.rem(z + k, sp)
        )
        c.start()
        s_copies.append(c)
    for k in range(sp):
        who = lax.rem(z - k + sp, sp)
        if k > 0:
            x_copies[k - 1].wait_recv()
        c = remote(
            x_ref if k == 0 else xs.at[who, :, slot], xs.at[who, :, slot],
            f_send.at[k], f_recv.at[k], "tp", lax.rem(t + 1, tp),
        )
        c.start()
        f_copies.append(c)
    own_x.wait()
    own_shift.wait()
    for c in own_w:
        c.wait()
    for c in w_copies:
        c.wait_recv()
    for k in range(sp):
        who = lax.rem(z - k + sp, sp)
        f_copies[k].wait_recv()
        at = pl.ds(pl.multiple_of(who * rows, rows), rows)
        for i in range(0, len(weights), 2):
            out = jnp.dot(
                xs[who], ws[:, i * cols : (i + 2) * cols], preferred_element_type=jnp.float32
            ).astype(jnp.bfloat16)
            p_ref[i, at, :] = out[:, :cols]
            p_ref[i + 1, at, :] = out[:, cols:]
        pre_ref[at, :] = jnp.dot(
            xs[who], gates_ref[...], preferred_element_type=jnp.float32
        )
    for c in s_copies:
        c.wait_recv()
    for c in x_copies + w_copies + s_copies + f_copies:
        c.wait_send()


def stick_kernel(offset_ref, p_ref, out_ref):
    rows = out_ref.shape[0]
    i = pl.program_id(0)
    lane = lax.broadcasted_iota(jnp.int32, (rows, out_ref.shape[1]), 1)
    heads = offset_ref.shape[0]
    size = out_ref.shape[1] // heads
    below = lax.broadcasted_iota(jnp.int32, (rows, rows), 0)
    across = lax.broadcasted_iota(jnp.int32, (rows, rows), 1)
    after = jnp.where(below >= across, 1.0, 0.0).astype(jnp.bfloat16)
    scale = size ** (-0.5)
    q = p_ref[0, pl.ds(pl.multiple_of(i * rows, rows), rows), :]
    queries = [
        jnp.where(lane // size == h, q, jnp.zeros_like(q)) for h in range(heads)
    ]

    def block(j, carry, masked):
        at = pl.ds(pl.multiple_of(j * rows, rows), rows)
        keys, values = p_ref[1, at, :], p_ref[2, at, :]
        new = []
        for h in range(heads):
            acc, later = carry[h]
            score = (
                lax.dot_general(
                    queries[h], keys, (((1,), (1,)), ((), ())),
                    preferred_element_type=jnp.float32,
                ) * scale + offset_ref[h]
            )
            skip = -(jnp.maximum(score, 0.0) + jnp.log(1.0 + jnp.exp(-jnp.abs(score))))
            if masked:
                skip = jnp.where(across < below, skip, 0.0)
            high = skip.astype(jnp.bfloat16)
            low = (skip - high.astype(jnp.float32)).astype(jnp.bfloat16)
            total = jnp.dot(high, after, preferred_element_type=jnp.float32) + jnp.dot(
                low, after, preferred_element_type=jnp.float32
            )
            weight = jnp.exp(score + total)
            if masked:
                weight = jnp.where(across < below, weight, 0.0)
            part = jnp.dot(
                weight.astype(jnp.bfloat16), values, preferred_element_type=jnp.float32
            )
            new.append((acc + part * jnp.exp(later), later + total[:, :1]))
        return tuple(new)

    start = tuple(
        (jnp.zeros(out_ref.shape, jnp.float32), jnp.zeros((rows, 1), jnp.float32))
        for h in range(heads)
    )
    carry = block(i, start, True)
    carry = lax.fori_loop(0, i, lambda n, c: block(i - 1 - n, c, False), carry)
    mixed = carry[0][0]
    for h in range(1, heads):
        mixed = jnp.where(lane // size == h, carry[h][0], mixed)
    out_ref[...] = mixed.astype(out_ref.dtype)


def halves(a):
    high = a.astype(jnp.bfloat16)
    return high, (a - high.astype(jnp.float32)).astype(jnp.bfloat16)


def product(a, b, dims=((1,), (0,))):
    def one(x, y):
        return lax.dot_general(x, y, (dims, ((), ())), preferred_element_type=jnp.float32)

    return one(a[0], b[0]) + (one(a[0], b[1]) + one(a[1], b[0]))


def delta_kernel(p_ref, decay_ref, strength_ref, gain_ref, out_ref, maps, adds):
    length, size = out_ref.shape
    span = BLOCK
    group = 4
    row = lax.broadcasted_iota(jnp.int32, (span, span), 0)
    col = lax.broadcasted_iota(jnp.int32, (span, span), 1)
    inclusive, strictly = col <= row, col < row
    lower = jnp.where(inclusive, 1.0, 0.0)
    unit = jnp.where(col == row, 1.0, 0.0)
    diagonal = lax.broadcasted_iota(jnp.int32, (size, size), 0) == lax.broadcasted_iota(
        jnp.int32, (size, size), 1
    )

    def silu(a):
        a = a.astype(jnp.float32)
        return a * (1.0 / (1.0 + jnp.exp(-a)))

    def unit_of(a):
        return a * lax.rsqrt(jnp.sum(a * a, axis=-1, keepdims=True) + NORM_EPS)

    def prepare(step, carry):
        blocks = []
        for b in range(group):
            at = pl.ds(pl.multiple_of((step * group + b) * span, span), span)
            q = unit_of(silu(p_ref[3, at, :])) * size ** (-0.5)
            k = unit_of(silu(p_ref[4, at, :]))
            v = silu(p_ref[5, at, :])
            decay = jnp.broadcast_to(decay_ref[at, :], (span, size))
            strength = strength_ref[at, :]
            cumulative = jnp.dot(lower, decay, precision=EXACT_MATMUL)
            narrow = cumulative[:, :span]
            spread = narrow - narrow.T
            table = jnp.where(inclusive, jnp.exp(jnp.where(inclusive, spread, 0.0)), 0.0)
            growth = jnp.exp(cumulative)
            last = cumulative[span - 1 : span, :]
            beta = k * strength
            ks = halves(k)
            near = product(halves(beta), ks, ((1,), (1,)))
            strict = jnp.where(strictly, near * table, 0.0)
            inside = product(halves(q), ks, ((1,), (1,))) * table
            right = jnp.concatenate([v * strength, beta * growth], axis=1)
            damped = k * jnp.exp(last - cumulative)
            blocks.append([strict, inside, right, damped, q * growth, jnp.exp(last)])
        inverses = [unit - b[0] for b in blocks]
        powers = [halves(b[0]) for b in blocks]
        for level in range(max(1, (span - 1).bit_length()) - 1):
            powers = [halves(product(a, a)) for a in powers]
            inverses = [a + product(halves(a), c) for a, c in zip(inverses, powers)]
        for b in range(group):
            strict, inside, right, damped, boosted, keep = blocks[b]
            solved = halves(product(halves(inverses[b]), halves(right)))
            state = product(halves(damped), solved, ((0,), (0,)))
            seen = product(halves(inside), solved)
            step_map = jnp.where(diagonal, keep, 0.0) - state[:, size:]
            high, low = halves(step_map)
            qhigh, qlow = halves(boosted - seen[:, size:])
            n = step * group + b
            maps[n, 0, :size, :] = high
            maps[n, 0, size:, :] = qhigh
            maps[n, 1, :size, :] = low
            maps[n, 1, size:, :] = qlow
            adds[n, :size, :] = state[:, :size]
            adds[n, size:, :] = seen[:, :size]
        return carry

    lax.fori_loop(0, length // (span * group), prepare, 0)

    def walk(n, memory):
        new = product((maps[n, 0], maps[n, 1]), halves(memory)) + adds[n]
        made = new[size:]
        made = made * lax.rsqrt(jnp.mean(made * made, axis=-1, keepdims=True) + NORM_EPS)
        at = pl.ds(pl.multiple_of(n * span, span), span)
        out_ref[at, :] = (made * gain_ref[...]).astype(out_ref.dtype)
        return new[:size]

    lax.fori_loop(0, length // span, walk, jnp.zeros((size, size), jnp.float32))


def output_kernel(
    stick_ref, delta_ref, sw_ref, dw_ref, out_ref,
    sticks, deltas, outgoing, incoming, own,
    a_send, a_recv, l_sem, c_send, c_recv,
):
    sp, tp = lax.axis_size("sp"), lax.axis_size("tp")
    z, t = lax.axis_index("sp"), lax.axis_index("tp")
    rows = sticks.shape[0]
    half = rows // tp
    pieces = ((stick_ref, sticks), (delta_ref, deltas))

    def source(ref, who):
        return ref.at[pl.ds(pl.multiple_of(who * rows, rows), rows), :]

    def slot(ref):
        cols = stick_ref.shape[1]
        return ref.at[:, pl.ds(pl.multiple_of(z * cols, cols), cols)]

    local = [
        pltpu.make_async_copy(source(a, z), slot(b), l_sem.at[i])
        for i, (a, b) in enumerate(pieces)
    ]
    for c in local:
        c.start()
    greet(("sp", "tp"))
    copies = []
    for k in range(1, sp):
        who = lax.rem(z + k, sp)
        for i, (a, b) in enumerate(pieces):
            c = remote(source(a, who), slot(b), a_send.at[k, i], a_recv.at[k, i], "sp", who)
            c.start()
            copies.append(c)
    for c in local:
        c.wait()
    for c in copies:
        c.wait_recv()
    chunks, width = outgoing.shape[0], outgoing.shape[2]
    mine = pl.ds(pl.multiple_of(t * half, half), half)
    partner = lax.rem(t + 1, tp)
    theirs = pl.ds(pl.multiple_of(partner * half, half), half)
    sends = []
    for c in range(chunks):
        columns = slice(c * width, (c + 1) * width)
        for which, target in ((theirs, outgoing), (mine, own)):
            target[c] = (
                jnp.dot(sticks[which, :], sw_ref[:, columns], preferred_element_type=jnp.float32)
                + jnp.dot(
                    deltas[which, :], dw_ref[:, columns], preferred_element_type=jnp.float32
                )
            ).astype(jnp.bfloat16)
        sends.append(
            remote(
                outgoing.at[c], incoming.at[c], c_send.at[c], c_recv.at[c], "tp", partner
            )
        )
        if c > 0:
            sends[c - 1].start()
    for c in copies:
        c.wait_send()
    sends[chunks - 1].start()
    for c in range(chunks):
        sends[c].wait_recv()
        out_ref[:, c * width : (c + 1) * width] = (
            own[c].astype(jnp.float32) + incoming[c].astype(jnp.float32)
        ).astype(out_ref.dtype)
    for c in sends:
        c.wait_send()


ANYWHERE = pl.BlockSpec(memory_space=pl.ANY)
ON_CORE = pl.BlockSpec(memory_space=pltpu.VMEM)


def on_device_heads(
    hidden_in, sb_query_w, sb_key_w, sb_value_w, sb_offset,
    delta_query_w, delta_key_w, delta_value_w, decay_w, write_w, write_bias,
    decay_log_scale, decay_shift, head_gain, sb_out_w, delta_out_w,
):
    sp, fs, tp = lax.axis_size("sp"), lax.axis_size("fs"), lax.axis_size("tp")
    z = lax.axis_index("sp")
    rows, half = hidden_in.shape[1:]
    width = half * tp
    length = rows * sp
    heads = decay_log_scale.shape[0]
    sb_heads = sb_offset.shape[0] // sp
    cols = sb_query_w.shape[1] // sp
    gates = jnp.concatenate([decay_w, write_w], axis=1)
    dma = pltpu.SemaphoreType.DMA
    projected, pre, shifts = pl.pallas_call(
        project_kernel,
        name="project",
        out_shape=(
            jax.ShapeDtypeStruct((6, length, cols), jnp.bfloat16),
            jax.ShapeDtypeStruct((length, 2 * heads), jnp.float32),
            jax.ShapeDtypeStruct((sp, heads, rows), jnp.float32),
        ),
        in_specs=[ANYWHERE] * 7 + [ON_CORE, ANYWHERE],
        out_specs=(ON_CORE, ON_CORE, ON_CORE),
        scratch_shapes=[
            pltpu.VMEM((sp, rows, width), jnp.bfloat16),
            pltpu.VMEM((width, 6 * cols), jnp.bfloat16),
            dma((sp,)), dma((sp,)), dma((sp,)), dma((sp,)),
            dma((fs, 6)), dma((fs, 6)), dma((sp,)), dma((sp,)), dma((2,)), dma((6,)),
        ],
        compiler_params=pltpu.CompilerParams(
            collective_id=0, has_side_effects=True, vmem_limit_bytes=40 * 2**20
        ),
    )(
        hidden_in.reshape(rows, half), sb_query_w, sb_key_w, sb_value_w,
        delta_query_w, delta_key_w, delta_value_w, gates, decay_shift.reshape(heads, rows),
    )

    def pick(a, start, count, axis):
        return lax.dynamic_slice_in_dim(a, start, count, axis)

    decay = (
        -jnp.exp(pick(decay_log_scale, z, 1, 0)) * jax.nn.softplus(pick(pre, z, 1, 1))
        + pick(shifts, z, 1, 1).reshape(length, 1)
    )
    strength = jax.nn.sigmoid(pick(pre, heads + z, 1, 1) + pick(write_bias, z, 1, 0))
    stick = pl.pallas_call(
        stick_kernel,
        name="stick",
        grid=(sp,),
        out_shape=jax.ShapeDtypeStruct((length, cols), jnp.bfloat16),
        in_specs=[
            pl.BlockSpec(memory_space=pltpu.SMEM),
            pl.BlockSpec((3, length, cols), lambda i: (0, 0, 0)),
        ],
        out_specs=pl.BlockSpec((rows, cols), lambda i: (i, 0)),
        compiler_params=pltpu.CompilerParams(vmem_limit_bytes=40 * 2**20),
    )(pick(sb_offset, z * sb_heads, sb_heads, 0), projected)
    delta = pl.pallas_call(
        delta_kernel,
        name="delta",
        out_shape=jax.ShapeDtypeStruct((length, cols), jnp.bfloat16),
        in_specs=[ON_CORE] * 4,
        out_specs=ON_CORE,
        scratch_shapes=[
            pltpu.VMEM((length // BLOCK, 2, cols + BLOCK, cols), jnp.bfloat16),
            pltpu.VMEM((length // BLOCK, cols + BLOCK, cols), jnp.float32),
        ],
        compiler_params=pltpu.CompilerParams(vmem_limit_bytes=40 * 2**20),
    )(projected, decay, strength, head_gain.reshape(1, -1))
    chunks = 4
    result = pl.pallas_call(
        output_kernel,
        name="output",
        out_shape=jax.ShapeDtypeStruct((rows // tp, width), jnp.bfloat16),
        in_specs=[ANYWHERE, ANYWHERE, ON_CORE, ON_CORE],
        out_specs=ON_CORE,
        scratch_shapes=[
            pltpu.VMEM((rows, cols * sp), jnp.bfloat16),
            pltpu.VMEM((rows, cols * sp), jnp.bfloat16),
            pltpu.VMEM((chunks, rows // tp, width // chunks), jnp.bfloat16),
            pltpu.VMEM((chunks, rows // tp, width // chunks), jnp.bfloat16),
            pltpu.VMEM((chunks, rows // tp, width // chunks), jnp.bfloat16),
            dma((sp, 2)), dma((sp, 2)), dma((2,)), dma((chunks,)), dma((chunks,)),
        ],
        compiler_params=pltpu.CompilerParams(
            collective_id=1, has_side_effects=True, vmem_limit_bytes=40 * 2**20
        ),
    )(stick, delta, sb_out_w, delta_out_w)
    return result.reshape(1, rows // tp, width)


def on_device(*inputs):
    delta_heads = inputs[11].shape[0]
    if delta_heads == lax.axis_size("sp") and inputs[4].shape[0] % delta_heads == 0:
        return on_device_heads(*inputs)
    return on_device_split(*inputs)


def solution(mesh):
    return jax.shard_map(
        on_device,
        mesh=mesh,
        in_specs=(
            P("fs", "sp", "tp"),
            P("fs", "tp"),
            P("fs", "tp"),
            P("fs", "tp"),
            P("tp"),
            P("fs", "tp"),
            P("fs", "tp"),
            P("fs", "tp"),
            P(None, "tp"),
            P(None, "tp"),
            P("tp"),
            P("tp"),
            P("fs", "tp", "sp"),
            P(),
            P("tp", None),
            P("tp", None),
        ),
        out_specs=P("fs", ("sp", "tp"), None),
        check_vma=False,
    )
```

```python
import jax
import jax.numpy as jnp
from jax import lax
from jax.experimental import pallas as pl
from jax.experimental.pallas import tpu as pltpu
from jax.sharding import PartitionSpec as P

MESH = pl.DeviceIdType.MESH
ALL_VMEM = 67043328

SB_DIM = 64
GDN_DIM = 128
BLOCK = 64


EXACT_MATMUL = lax.Precision.HIGHEST
NORM_EPS = 1e-06


def carried_in(value, axis, combine, identity):
    devices, index = (lax.axis_size(axis), lax.axis_index(axis))
    everything = jax.tree.map(
        lambda part, kind: lax.all_gather(part.astype(kind), axis),
        value,
        (jnp.bfloat16, jnp.bfloat16),
    )
    start = jax.tree.map(
        lambda part, zero: jnp.broadcast_to(jnp.asarray(zero, part.dtype), part.shape),
        value,
        identity,
    )

    def lap(k, before):
        reached = k < index
        new = combine(
            before, jax.tree.map(lambda part, own: part[k].astype(own.dtype), everything, value)
        )
        return jax.tree.map(lambda a, b: jnp.where(reached, a, b), new, before)

    return lax.fori_loop(0, devices, lap, start)


def unit_lower_inverse(strict_part):
    order_size = strict_part.shape[-1]
    powered = strict_part
    inverse = jnp.eye(order_size, dtype=strict_part.dtype) - strict_part
    for repeat_number in range(max(1, (order_size - 1).bit_length()) - 1):
        powered = jnp.einsum("...ij,...jk->...ik", powered, powered, precision=EXACT_MATMUL)
        inverse = inverse + jnp.einsum(
            "...ij,...jk->...ik", inverse, powered, precision=EXACT_MATMUL
        )
    return inverse


def to_blocks(row_data, block_span):
    blocks_count = row_data.shape[0] // block_span
    shaped = row_data.reshape((blocks_count, block_span) + row_data.shape[1:])
    return jnp.swapaxes(shaped, 1, 2)


def from_blocks(blocked):
    swapped = jnp.swapaxes(blocked, 1, 2)
    return swapped.reshape((-1,) + swapped.shape[2:])


def unit_rows(vectors):
    return vectors * lax.rsqrt(jnp.sum(vectors * vectors, axis=-1, keepdims=True) + NORM_EPS)


def delta_inputs(
    query_proj,
    key_proj,
    value_proj,
    decay_pre,
    write_pre,
    write_bias,
    decay_log_scale,
    shift_rows,
    head_count,
    head_size,
):
    query_act = jax.nn.silu(query_proj.astype(jnp.float32)).reshape(-1, head_count, head_size)
    key_act = jax.nn.silu(key_proj.astype(jnp.float32)).reshape(-1, head_count, head_size)
    value_rows = jax.nn.silu(value_proj.astype(jnp.float32)).reshape(-1, head_count, head_size)
    queries = unit_rows(query_act) * head_size ** (-0.5)
    key_rows = unit_rows(key_act)
    log_decay = -jnp.exp(decay_log_scale) * jax.nn.softplus(decay_pre) + shift_rows
    strength = jax.nn.sigmoid(write_pre + write_bias)
    return (queries, key_rows, value_rows, log_decay, strength)


def delta_prepare(queries, key_rows, value_rows, log_decay, strength):
    block_span = queries.shape[2]
    cumulative = jnp.cumsum(log_decay, axis=-1)
    row_place = lax.broadcasted_iota(jnp.int32, (block_span, block_span), 0)
    col_place = lax.broadcasted_iota(jnp.int32, (block_span, block_span), 1)
    inclusive = col_place <= row_place
    strictly = col_place < row_place
    spread = cumulative[..., :, None] - cumulative[..., None, :]
    decay_table = jnp.where(inclusive, jnp.exp(jnp.where(inclusive, spread, 0.0)), 0.0)
    keys_beta = key_rows * strength[..., None]
    lower_part = jnp.where(
        strictly,
        jnp.einsum("nhik,nhjk->nhij", keys_beta, key_rows, precision=EXACT_MATMUL) * decay_table,
        0.0,
    )
    inverse = unit_lower_inverse(lower_part)
    growth = jnp.exp(cumulative)
    state_updates = jnp.einsum(
        "nhij,nhjv->nhiv", inverse, value_rows * strength[..., None], precision=EXACT_MATMUL
    )
    erase_term = jnp.einsum(
        "nhij,nhjk->nhik", inverse, keys_beta * growth[..., None], precision=EXACT_MATMUL
    )
    inside_block = (
        jnp.einsum("nhik,nhjk->nhij", queries, key_rows, precision=EXACT_MATMUL) * decay_table
    )
    boosted_query = queries * growth[..., None]
    damped_keys = key_rows * jnp.exp(cumulative[..., -1:] - cumulative)[..., None]
    decay_per_block = jnp.exp(cumulative[..., -1])
    return (state_updates, erase_term, inside_block, boosted_query, damped_keys, decay_per_block)


def delta_step(memory_state, inputs):
    state_updates, erase_term, inside_block, boosted_query, damped_keys, decay_per_block = inputs
    fixed_values = state_updates - jnp.einsum(
        "mzq,mqc->mzc", erase_term, memory_state, precision=EXACT_MATMUL
    )
    produced_rows = jnp.einsum(
        "mzq,mqc->mzc", boosted_query, memory_state, precision=EXACT_MATMUL
    ) + jnp.einsum("efq,eqn->efn", inside_block, fixed_values, precision=EXACT_MATMUL)
    memory_state = memory_state * decay_per_block[:, None, None] + jnp.einsum(
        "wam,waz->wmz", damped_keys, fixed_values, precision=EXACT_MATMUL
    )
    return (memory_state, produced_rows)


def transition_step(carried, inputs):
    memory_state, transfer = carried
    state_updates, erase_term, inside_block, boosted_query, damped_keys, decay_per_block = inputs
    fixed_values = state_updates - jnp.einsum(
        "mzq,mqc->mzc", erase_term, memory_state, precision=EXACT_MATMUL
    )
    coupling = jnp.einsum("hik,hil->hkl", damped_keys, erase_term, precision=EXACT_MATMUL)
    memory_state = memory_state * decay_per_block[:, None, None] + jnp.einsum(
        "wam,waz->wmz", damped_keys, fixed_values, precision=EXACT_MATMUL
    )
    transfer = transfer * decay_per_block[:, None, None] - jnp.einsum(
        "hkl,hlm->hkm", coupling, transfer, precision=EXACT_MATMUL
    )
    return ((memory_state, transfer), None)


def compose(prior_blocks, following_blocks):
    joined_map = jnp.einsum(
        "hkl,hlm->hkm", following_blocks[0], prior_blocks[0], precision=EXACT_MATMUL
    )
    joined_state = (
        jnp.einsum("djo,dog->djg", following_blocks[0], prior_blocks[1], precision=EXACT_MATMUL)
        + following_blocks[1]
    )
    return (joined_map, joined_state)


def stick_block(queries, key_rows, value_rows, query_place, key_place, offsets):
    scale_factor = queries.shape[-1] ** (-0.5)
    scores = (
        jnp.einsum("qhd,khd->hqk", queries, key_rows, preferred_element_type=jnp.float32)
        * scale_factor
        + offsets[:, None, None]
    )
    visible = key_place[None, :] < query_place[:, None]
    skipped = jnp.where(visible, jax.nn.log_sigmoid(-scores), 0.0)
    beyond = lax.cumsum(skipped, axis=2, reverse=True) - skipped
    weights = jnp.where(visible, jnp.exp(jax.nn.log_sigmoid(scores) + beyond), 0.0).astype(
        jnp.bfloat16
    )
    partial_value = jnp.einsum(
        "hqk,khd->qhd", weights, value_rows, preferred_element_type=jnp.float32
    )
    return (partial_value, jnp.sum(skipped, axis=2).T)


def stick_combine(partials, totals):
    beyond = jnp.cumsum(totals[::-1], axis=0)[::-1] - totals
    return jnp.sum(partials * jnp.exp(beyond)[..., None], axis=0)


def on_device_split(
    hidden_in,
    sb_query_w,
    sb_key_w,
    sb_value_w,
    sb_offset,
    delta_query_w,
    delta_key_w,
    delta_value_w,
    decay_w,
    write_w,
    write_bias,
    decay_log_scale,
    decay_shift,
    head_gain,
    sb_out_w,
    delta_out_w,
):
    token_rows = hidden_in.shape[1]
    local_in = hidden_in.reshape(token_rows, hidden_in.shape[2])
    gathered = (
        lax.all_gather(sb_query_w, "fs", axis=0, tiled=True),
        lax.all_gather(sb_key_w, "fs", axis=0, tiled=True),
        lax.all_gather(sb_value_w, "fs", axis=0, tiled=True),
        lax.all_gather(delta_query_w, "fs", axis=0, tiled=True),
        lax.all_gather(delta_key_w, "fs", axis=0, tiled=True),
        lax.all_gather(delta_value_w, "fs", axis=0, tiled=True),
    )
    in_weights = tuple(gathered) + (decay_w, write_w)
    portion = lax.all_gather(local_in, "tp", axis=1, tiled=True)
    projected = tuple(
        (jnp.dot(portion, weight, preferred_element_type=jnp.float32) for weight in in_weights)
    )
    sb_heads = sb_offset.shape[0]
    delta_heads = decay_log_scale.shape[0]
    sb_query = projected[0].astype(jnp.bfloat16).reshape(token_rows, sb_heads, SB_DIM)
    sb_keys = projected[1].astype(jnp.bfloat16)
    sb_values = projected[2].astype(jnp.bfloat16)
    shift_rows = decay_shift.reshape(delta_heads, token_rows).T
    queries, key_rows, value_rows, log_decay, strength = delta_inputs(
        projected[3].astype(jnp.bfloat16),
        projected[4].astype(jnp.bfloat16),
        projected[5].astype(jnp.bfloat16),
        projected[6],
        projected[7],
        write_bias,
        decay_log_scale,
        shift_rows,
        delta_heads,
        GDN_DIM,
    )
    prepared = delta_prepare(
        to_blocks(queries, BLOCK),
        to_blocks(key_rows, BLOCK),
        to_blocks(value_rows, BLOCK),
        to_blocks(log_decay, BLOCK),
        to_blocks(strength, BLOCK),
    )
    identity_map = jnp.broadcast_to(
        jnp.eye(GDN_DIM, dtype=jnp.float32), (delta_heads, GDN_DIM, GDN_DIM)
    )
    empty_state = jnp.zeros((delta_heads, GDN_DIM, GDN_DIM), jnp.float32)
    (local_end, local_map), unused_out = lax.scan(
        transition_step, (empty_state, identity_map), prepared
    )
    own_first = lax.axis_index("sp") * token_rows
    query_place = own_first + lax.iota(jnp.int32, token_rows)
    sp_count = lax.axis_size("sp")
    slot_out = jnp.zeros((sp_count, token_rows, sb_heads, SB_DIM), jnp.float32)
    slot_total = jnp.zeros((sp_count, token_rows, sb_heads), jnp.float32)

    def absorb(slot_arrays, address_portion, value_part, shard_first):

        def active(current):
            partial_value, totals = stick_block(
                sb_query,
                address_portion.reshape(token_rows, sb_heads, SB_DIM),
                value_part.reshape(token_rows, sb_heads, SB_DIM),
                query_place,
                shard_first + lax.iota(jnp.int32, token_rows),
                sb_offset,
            )
            slot_index = shard_first // token_rows
            return (
                lax.dynamic_update_index_in_dim(current[0], partial_value, slot_index, 0),
                lax.dynamic_update_index_in_dim(current[1], totals, slot_index, 0),
            )

        def inactive(current):
            return current

        usable = jnp.logical_and(shard_first >= 0, shard_first <= own_first)
        return lax.cond(usable, active, inactive, slot_arrays)

    key_block = lax.all_gather(sb_keys, "sp", axis=0, tiled=True)
    value_block = lax.all_gather(sb_values, "sp", axis=0, tiled=True)

    def per_shard(shard_number, current):
        row_begin = shard_number * token_rows
        return absorb(
            current,
            lax.dynamic_slice_in_dim(key_block, row_begin, token_rows, 0),
            lax.dynamic_slice_in_dim(value_block, row_begin, token_rows, 0),
            row_begin,
        )

    slot_arrays = lax.fori_loop(
        0, key_block.shape[0] // token_rows, per_shard, (slot_out, slot_total)
    )
    unused_map, incoming = carried_in(
        (local_map, local_end), "sp", compose, (identity_map, empty_state)
    )
    sb_mixed = (
        stick_combine(slot_arrays[0], slot_arrays[1])
        .astype(jnp.bfloat16)
        .reshape(token_rows, sb_heads * SB_DIM)
    )
    unused_end, produced_rows = lax.scan(delta_step, incoming, prepared)
    produced_rows = from_blocks(produced_rows)
    normed = (
        produced_rows
        * lax.rsqrt(jnp.mean(produced_rows * produced_rows, axis=-1, keepdims=True) + NORM_EPS)
        * head_gain
    )
    delta_mixed = normed.astype(jnp.bfloat16).reshape(token_rows, delta_heads * GDN_DIM)
    result = lax.psum_scatter(
        (
            jnp.dot(sb_mixed, sb_out_w, preferred_element_type=jnp.float32)
            + jnp.dot(delta_mixed, delta_out_w, preferred_element_type=jnp.float32)
        ).astype(jnp.bfloat16),
        "tp",
        scatter_dimension=0,
        tiled=True,
    ).astype(jnp.float32)
    return result.astype(jnp.bfloat16).reshape(1, result.shape[0], result.shape[1])


def remote(src, dst, send, recv, axis, index):
    return pltpu.make_async_remote_copy(
        src_ref=src, dst_ref=dst, send_sem=send, recv_sem=recv,
        device_id={axis: index}, device_id_type=MESH,
    )


def greet(axes):
    barrier = pltpu.get_barrier_semaphore()
    count = 0
    for axis in axes:
        size, me = lax.axis_size(axis), lax.axis_index(axis)
        for k in range(1, size):
            pl.semaphore_signal(
                barrier, inc=1, device_id={axis: lax.rem(me + k, size)}, device_id_type=MESH
            )
            count += 1
    pl.semaphore_wait(barrier, count)


def project_kernel(
    x_ref, w0, w1, w2, w3, w4, w5, decay_w_ref, write_w_ref, shift_ref,
    p_ref, decay_pre_ref, write_pre_ref, shifts_ref,
    xs, ws, decay_w, write_w,
    x_send, x_recv, f_send, f_recv, w_send, w_recv, s_send, s_recv, l_sem, lw_sem,
):
    weights = (w0, w1, w2, w3, w4, w5)
    sp, tp = lax.axis_size("sp"), lax.axis_size("tp")
    z, f, t = lax.axis_index("sp"), lax.axis_index("fs"), lax.axis_index("tp")
    rows, half = x_ref.shape
    depth = w0.shape[0]
    cols = ws.shape[1] // len(weights)
    parts = x_send.shape[2]
    slot = pl.ds(pl.multiple_of(t * half, half), half)
    local = [
        pltpu.make_async_copy(x_ref, xs.at[z, :, slot], l_sem.at[0]),
        pltpu.make_async_copy(shift_ref, shifts_ref.at[z], l_sem.at[1]),
        pltpu.make_async_copy(decay_w_ref, decay_w, l_sem.at[2]),
        pltpu.make_async_copy(write_w_ref, write_w, l_sem.at[3]),
    ]

    def w_src(i):
        return weights[i].at[:, pl.ds(pl.multiple_of(z * cols, cols), cols)]

    def w_at(i, who):
        return ws.at[pl.ds(pl.multiple_of(who * depth, depth), depth), pl.ds(i * cols, cols)]

    local += [
        pltpu.make_async_copy(w_src(i), w_at(i, f), lw_sem.at[i]) for i in range(len(weights))
    ]
    for c in local:
        c.start()
    greet(("sp", "fs", "tp"))

    near = (f + 1 - 2 * (f % 2), f + 2 - 4 * (f // 2))
    count = len(weights)
    orders = (tuple(range(count)), tuple(range(count // 2, count)) + tuple(range(count // 2)))

    def x_copy(way, step, part):
        block = z - (step - 1) if way == 0 else z + (step - 1)
        piece = pl.ds(part * (rows // parts), rows // parts)
        there = xs.at[block, piece, slot]
        return remote(
            x_ref.at[piece, :] if step == 1 else there, there,
            x_send.at[way, step, part], x_recv.at[way, step, part],
            "sp", z + 1 if way == 0 else z - 1,
        )

    def onward(way):
        return z + 1 < sp if way == 0 else z > 0

    def comes(way, step):
        return z >= step if way == 0 else z + step < sp

    def sends(way, step):
        return jnp.logical_and(onward(way), comes(way, step - 1))

    def forward(way, step, part):
        block = z - step if way == 0 else z + step
        piece = pl.ds(part * (rows // parts), rows // parts)
        there = xs.at[block, piece, slot]
        return remote(
            x_ref.at[piece, :] if step == 0 else there, there,
            f_send.at[way, step, part], f_recv.at[way, step, part], "tp", lax.rem(t + 1, tp),
        )

    for part in range(parts):
        for way in range(2):
            @pl.when(onward(way))
            def _():
                x_copy(way, 1, part).start()

    w_copies = {}
    for order_at in range(count):
        for side in range(2):
            i = orders[side][order_at]
            c = remote(
                w_src(i), w_at(i, f), w_send.at[side, i], w_recv.at[side, i], "fs", near[side]
            )
            c.start()
            w_copies[side, i] = c
    s_copies = []
    for k in range(1, sp):
        c = remote(
            shift_ref, shifts_ref.at[z], s_send.at[k], s_recv.at[k], "sp", lax.rem(z + k, sp)
        )
        c.start()
        s_copies.append(c)
    for part in range(parts):
        forward(0, 0, part).start()

    relays = []

    def relay(position):
        for side in range(2):
            i = orders[side][position]
            w_copies[side, i].wait_recv()
            there = w_at(i, near[side])
            c = remote(
                there, there, w_send.at[2 + side, i], w_recv.at[2 + side, i],
                "fs", near[1 - side],
            )
            c.start()
            relays.append(c)

    for step in range(1, sp):
        relay(step - 1)
        for part in range(parts):
            for way in range(2):
                @pl.when(comes(way, step))
                def _():
                    x_copy(way, step, part).wait_recv()
                    forward(way, step, part).start()
                    if step + 1 < sp:
                        @pl.when(onward(way))
                        def _():
                            x_copy(way, step + 1, part).start()
    for position in range(sp - 1, count // 2):
        relay(position)
    for c in local:
        c.wait()
    for side in range(2):
        for position in range(count // 2, count):
            w_copies[side, orders[side][position]].wait_recv()
    for c in relays:
        c.wait_recv()

    def project(block):
        at = pl.ds(pl.multiple_of(block * rows, rows), rows)
        for i in range(0, count, 2):
            out = jnp.dot(
                xs[block], ws[:, i * cols : (i + 2) * cols], preferred_element_type=jnp.float32
            ).astype(jnp.bfloat16)
            p_ref[i, at, :] = out[:, :cols]
            p_ref[i + 1, at, :] = out[:, cols:]
        decay_pre_ref[at, :] = lax.dot_general(
            xs[block], decay_w[...], (((1,), (1,)), ((), ())),
            preferred_element_type=jnp.float32,
        )
        write_pre_ref[at, :] = lax.dot_general(
            xs[block], write_w[...], (((1,), (1,)), ((), ())),
            preferred_element_type=jnp.float32,
        )

    for part in range(parts):
        forward(0, 0, part).wait_recv()
    project(z)
    for step in range(1, sp):
        for way in range(2):
            @pl.when(comes(way, step))
            def _():
                for part in range(parts):
                    forward(way, step, part).wait_recv()
                project(z - step if way == 0 else z + step)
    for c in s_copies:
        c.wait_recv()
    for c in list(w_copies.values()) + relays + s_copies:
        c.wait_send()
    for part in range(parts):
        forward(0, 0, part).wait_send()
        for step in range(1, sp):
            for way in range(2):
                @pl.when(sends(way, step))
                def _():
                    x_copy(way, step, part).wait_send()

                @pl.when(comes(way, step))
                def _():
                    forward(way, step, part).wait_send()


def stick_kernel(offset_ref, p_ref, out_ref):
    rows = out_ref.shape[0]
    i = pl.program_id(0)
    lane = lax.broadcasted_iota(jnp.int32, (rows, out_ref.shape[1]), 1)
    heads = offset_ref.shape[0]
    size = out_ref.shape[1] // heads
    below = lax.broadcasted_iota(jnp.int32, (rows, rows), 0)
    across = lax.broadcasted_iota(jnp.int32, (rows, rows), 1)
    after = jnp.where(below >= across, 1.0, 0.0).astype(jnp.bfloat16)
    scale = size ** (-0.5)
    q = p_ref[0, pl.ds(pl.multiple_of(i * rows, rows), rows), :]
    queries = [
        jnp.where(lane // size == h, q, jnp.zeros_like(q)) for h in range(heads)
    ]

    def block(j, carry, masked):
        at = pl.ds(pl.multiple_of(j * rows, rows), rows)
        keys, values = p_ref[1, at, :], p_ref[2, at, :]
        new = []
        for h in range(heads):
            acc, later = carry[h]
            score = (
                lax.dot_general(
                    queries[h], keys, (((1,), (1,)), ((), ())),
                    preferred_element_type=jnp.float32,
                ) * scale + offset_ref[h]
            )
            skip = -(jnp.maximum(score, 0.0) + jnp.log(1.0 + jnp.exp(-jnp.abs(score))))
            if masked:
                skip = jnp.where(across < below, skip, 0.0)
            high = skip.astype(jnp.bfloat16)
            low = (skip - high.astype(jnp.float32)).astype(jnp.bfloat16)
            total = jnp.dot(high, after, preferred_element_type=jnp.float32) + jnp.dot(
                low, after, preferred_element_type=jnp.float32
            )
            weight = jnp.exp(score + total)
            if masked:
                weight = jnp.where(across < below, weight, 0.0)
            part = jnp.dot(
                weight.astype(jnp.bfloat16), values, preferred_element_type=jnp.float32
            )
            new.append((acc + part * jnp.exp(later), later + total[:, :1]))
        return tuple(new)

    start = tuple(
        (jnp.zeros(out_ref.shape, jnp.float32), jnp.zeros((rows, 1), jnp.float32))
        for h in range(heads)
    )
    carry = block(i, start, True)
    carry = lax.fori_loop(0, i, lambda n, c: block(i - 1 - n, c, False), carry)
    mixed = carry[0][0]
    for h in range(1, heads):
        mixed = jnp.where(lane // size == h, carry[h][0], mixed)
    out_ref[...] = mixed.astype(out_ref.dtype)


def halves(a):
    high = a.astype(jnp.bfloat16)
    return high, (a - high.astype(jnp.float32)).astype(jnp.bfloat16)


def product(a, b, dims=((1,), (0,))):
    def one(x, y):
        return lax.dot_general(x, y, (dims, ((), ())), preferred_element_type=jnp.float32)

    return one(a[0], b[0]) + (one(a[0], b[1]) + one(a[1], b[0]))


def delta_kernel(
    decay_scale_ref, write_bias_ref, p_ref, decay_pre_ref, write_pre_ref, shifts_ref, gain_ref,
    out_ref, maps, adds, decays, strengths,
):
    z = lax.axis_index("sp")
    length, size = out_ref.shape
    span = BLOCK
    group = 4
    row = lax.broadcasted_iota(jnp.int32, (span, span), 0)
    col = lax.broadcasted_iota(jnp.int32, (span, span), 1)
    inclusive, strictly = col <= row, col < row
    lower = jnp.where(inclusive, 1.0, 0.0)
    unit = jnp.where(col == row, 1.0, 0.0)
    diagonal = lax.broadcasted_iota(jnp.int32, (size, size), 0) == lax.broadcasted_iota(
        jnp.int32, (size, size), 1
    )

    def silu(a):
        a = a.astype(jnp.float32)
        return a * (1.0 / (1.0 + jnp.exp(-a)))

    def unit_of(a):
        return a * lax.rsqrt(jnp.sum(a * a, axis=-1, keepdims=True) + NORM_EPS)

    heads = decay_pre_ref.shape[1]
    rows = shifts_ref.shape[2]
    mine = lax.broadcasted_iota(jnp.int32, (rows, heads), 1) == z
    square = lax.broadcasted_iota(jnp.int32, (rows, rows), 0) == lax.broadcasted_iota(
        jnp.int32, (rows, rows), 1
    )
    rate = jnp.exp(jnp.full((rows, 1), decay_scale_ref[z], jnp.float32))
    for part in range(length // rows):
        at = slice(part * rows, (part + 1) * rows)

        def chosen(ref):
            return jnp.sum(jnp.where(mine, ref[at, :], 0.0), axis=1, keepdims=True)

        shift = jnp.sum(
            jnp.where(square, shifts_ref[part, pl.ds(z, 1), :], 0.0), axis=1, keepdims=True
        )
        pre = chosen(decay_pre_ref)
        soft = jnp.maximum(pre, 0.0) + jnp.log(1.0 + jnp.exp(-jnp.abs(pre)))
        decays[at, :] = shift - rate * soft
        write = chosen(write_pre_ref) + write_bias_ref[z]
        strengths[at, :] = 1.0 / (1.0 + jnp.exp(-write))

    def prepare(step, carry):
        blocks = []
        for b in range(group):
            at = pl.ds(pl.multiple_of((step * group + b) * span, span), span)
            q = unit_of(silu(p_ref[3, at, :])) * size ** (-0.5)
            k = unit_of(silu(p_ref[4, at, :]))
            v = silu(p_ref[5, at, :])
            decay = jnp.broadcast_to(decays[at, :], (span, size))
            strength = strengths[at, :]
            cumulative = jnp.dot(lower, decay, precision=EXACT_MATMUL)
            narrow = cumulative[:, :span]
            spread = narrow - narrow.T
            table = jnp.where(inclusive, jnp.exp(jnp.where(inclusive, spread, 0.0)), 0.0)
            growth = jnp.exp(cumulative)
            last = cumulative[span - 1 : span, :]
            beta = k * strength
            ks = halves(k)
            near = product(halves(beta), ks, ((1,), (1,)))
            strict = jnp.where(strictly, near * table, 0.0)
            inside = product(halves(q), ks, ((1,), (1,))) * table
            right = jnp.concatenate([v * strength, beta * growth], axis=1)
            damped = k * jnp.exp(last - cumulative)
            blocks.append([strict, inside, right, damped, q * growth, jnp.exp(last)])
        inverses = [unit - b[0] for b in blocks]
        powers = [halves(b[0]) for b in blocks]
        for level in range(max(1, (span - 1).bit_length()) - 1):
            powers = [halves(product(a, a)) for a in powers]
            inverses = [a + product(halves(a), c) for a, c in zip(inverses, powers)]
        for b in range(group):
            strict, inside, right, damped, boosted, keep = blocks[b]
            solved = halves(product(halves(inverses[b]), halves(right)))
            state = product(halves(damped), solved, ((0,), (0,)))
            seen = product(halves(inside), solved)
            step_map = jnp.where(diagonal, keep, 0.0) - state[:, size:]
            high, low = halves(step_map)
            qhigh, qlow = halves(boosted - seen[:, size:])
            n = step * group + b
            maps[n, 0, :size, :] = high
            maps[n, 0, size:, :] = qhigh
            maps[n, 1, :size, :] = low
            maps[n, 1, size:, :] = qlow
            adds[n, :size, :] = state[:, :size]
            adds[n, size:, :] = seen[:, :size]
        return carry

    lax.fori_loop(0, length // (span * group), prepare, 0)

    def walk(n, memory):
        new = product((maps[n, 0], maps[n, 1]), halves(memory)) + adds[n]
        made = new[size:]
        made = made * lax.rsqrt(jnp.mean(made * made, axis=-1, keepdims=True) + NORM_EPS)
        at = pl.ds(pl.multiple_of(n * span, span), span)
        out_ref[at, :] = (made * gain_ref[...]).astype(out_ref.dtype)
        return new[:size]

    lax.fori_loop(0, length // span, walk, jnp.zeros((size, size), jnp.float32))


def output_kernel(
    stick_ref, delta_ref, sw_hbm, dw_hbm, out_ref,
    sticks, deltas, sw_ref, dw_ref, outgoing, incoming, own,
    a_send, a_recv, l_sem, c_send, c_recv,
):
    sp, tp = lax.axis_size("sp"), lax.axis_size("tp")
    z, t = lax.axis_index("sp"), lax.axis_index("tp")
    rows = sticks.shape[0]
    half = rows // tp
    pieces = ((stick_ref, sticks), (delta_ref, deltas))

    def source(ref, who):
        return ref.at[pl.ds(pl.multiple_of(who * rows, rows), rows), :]

    def slot(ref):
        cols = stick_ref.shape[1]
        return ref.at[:, pl.ds(pl.multiple_of(z * cols, cols), cols)]

    local = [
        pltpu.make_async_copy(source(a, z), slot(b), l_sem.at[i])
        for i, (a, b) in enumerate(pieces)
    ]
    local += [
        pltpu.make_async_copy(sw_hbm, sw_ref, l_sem.at[2]),
        pltpu.make_async_copy(dw_hbm, dw_ref, l_sem.at[3]),
    ]
    for c in local:
        c.start()
    greet(("sp", "tp"))
    copies = []
    for k in range(1, sp):
        who = lax.rem(z + k, sp)
        for i, (a, b) in enumerate(pieces):
            c = remote(source(a, who), slot(b), a_send.at[k, i], a_recv.at[k, i], "sp", who)
            c.start()
            copies.append(c)
    for c in local:
        c.wait()
    for c in copies:
        c.wait_recv()
    chunks, width = outgoing.shape[0], outgoing.shape[2]
    mine = pl.ds(pl.multiple_of(t * half, half), half)
    partner = lax.rem(t + 1, tp)
    theirs = pl.ds(pl.multiple_of(partner * half, half), half)
    sends = []
    for c in range(chunks):
        columns = slice(c * width, (c + 1) * width)
        for which, target in ((theirs, outgoing), (mine, own)):
            target[c] = (
                jnp.dot(sticks[which, :], sw_ref[:, columns], preferred_element_type=jnp.float32)
                + jnp.dot(
                    deltas[which, :], dw_ref[:, columns], preferred_element_type=jnp.float32
                )
            ).astype(jnp.bfloat16)
        sends.append(
            remote(
                outgoing.at[c], incoming.at[c], c_send.at[c], c_recv.at[c], "tp", partner
            )
        )
        if c > 0:
            sends[c - 1].start()
    for c in copies:
        c.wait_send()
    sends[chunks - 1].start()
    for c in range(chunks):
        sends[c].wait_recv()
        out_ref[:, c * width : (c + 1) * width] = (
            own[c].astype(jnp.float32) + incoming[c].astype(jnp.float32)
        ).astype(out_ref.dtype)
    for c in sends:
        c.wait_send()


ANYWHERE = pl.BlockSpec(memory_space=pltpu.HBM)
ON_CORE = pl.BlockSpec(memory_space=pltpu.VMEM)


def on_device_heads(
    hidden_in, sb_query_w, sb_key_w, sb_value_w, sb_offset,
    delta_query_w, delta_key_w, delta_value_w, decay_w, write_w, write_bias,
    decay_log_scale, decay_shift, head_gain, sb_out_w, delta_out_w,
):
    sp, fs, tp = lax.axis_size("sp"), lax.axis_size("fs"), lax.axis_size("tp")
    z = lax.axis_index("sp")
    rows, half = hidden_in.shape[1:]
    width = half * tp
    length = rows * sp
    heads = decay_log_scale.shape[0]
    sb_heads = sb_offset.shape[0] // sp
    cols = sb_query_w.shape[1] // sp
    parts = 2
    dma = pltpu.SemaphoreType.DMA
    projected, decay_pre, write_pre, shifts = pl.pallas_call(
        project_kernel,
        name="project",
        out_shape=(
            jax.ShapeDtypeStruct((6, length, cols), jnp.bfloat16),
            jax.ShapeDtypeStruct((length, heads), jnp.float32),
            jax.ShapeDtypeStruct((length, heads), jnp.float32),
            jax.ShapeDtypeStruct((sp, heads, rows), jnp.float32),
        ),
        in_specs=[ANYWHERE] * 10,
        out_specs=(ON_CORE,) * 4,
        scratch_shapes=[
            pltpu.VMEM((sp, rows, width), jnp.bfloat16),
            pltpu.VMEM((width, 6 * cols), jnp.bfloat16),
            pltpu.VMEM((heads, width), jnp.bfloat16),
            pltpu.VMEM((heads, width), jnp.bfloat16),
            dma((2, sp, parts)), dma((2, sp, parts)), dma((2, sp, parts)), dma((2, sp, parts)),
            dma((fs, 6)), dma((fs, 6)), dma((sp,)), dma((sp,)), dma((4,)), dma((6,)),
        ],
        compiler_params=pltpu.CompilerParams(
            collective_id=0, has_side_effects=True, vmem_limit_bytes=ALL_VMEM
        ),
    )(
        hidden_in.reshape(rows, half), sb_query_w, sb_key_w, sb_value_w,
        delta_query_w, delta_key_w, delta_value_w, decay_w.T, write_w.T, decay_shift.reshape(heads, rows),
    )

    def pick(a, start, count, axis):
        return lax.dynamic_slice_in_dim(a, start, count, axis)

    stick = pl.pallas_call(
        stick_kernel,
        name="stick",
        grid=(sp,),
        out_shape=jax.ShapeDtypeStruct((length, cols), jnp.bfloat16),
        in_specs=[
            pl.BlockSpec(memory_space=pltpu.SMEM),
            pl.BlockSpec((3, length, cols), lambda i: (0, 0, 0)),
        ],
        out_specs=pl.BlockSpec((rows, cols), lambda i: (i, 0)),
        compiler_params=pltpu.CompilerParams(vmem_limit_bytes=40 * 2**20),
    )(pick(sb_offset, z * sb_heads, sb_heads, 0), projected)
    delta = pl.pallas_call(
        delta_kernel,
        name="delta",
        out_shape=jax.ShapeDtypeStruct((length, cols), jnp.bfloat16),
        in_specs=[pl.BlockSpec(memory_space=pltpu.SMEM)] * 2 + [ON_CORE] * 5,
        out_specs=ON_CORE,
        scratch_shapes=[
            pltpu.VMEM((length // BLOCK, 2, cols + BLOCK, cols), jnp.bfloat16),
            pltpu.VMEM((length // BLOCK, cols + BLOCK, cols), jnp.float32),
            pltpu.VMEM((length, 1), jnp.float32),
            pltpu.VMEM((length, 1), jnp.float32),
        ],
        compiler_params=pltpu.CompilerParams(vmem_limit_bytes=40 * 2**20),
    )(
        decay_log_scale, write_bias, projected, decay_pre, write_pre, shifts,
        head_gain.reshape(1, -1),
    )
    chunks = 4
    result = pl.pallas_call(
        output_kernel,
        name="output",
        out_shape=jax.ShapeDtypeStruct((rows // tp, width), jnp.bfloat16),
        in_specs=[ON_CORE, ON_CORE, ANYWHERE, ANYWHERE],
        out_specs=ON_CORE,
        scratch_shapes=[
            pltpu.VMEM((rows, cols * sp), jnp.bfloat16),
            pltpu.VMEM((rows, cols * sp), jnp.bfloat16),
            pltpu.VMEM(sb_out_w.shape, jnp.bfloat16),
            pltpu.VMEM(delta_out_w.shape, jnp.bfloat16),
            pltpu.VMEM((chunks, rows // tp, width // chunks), jnp.bfloat16),
            pltpu.VMEM((chunks, rows // tp, width // chunks), jnp.bfloat16),
            pltpu.VMEM((chunks, rows // tp, width // chunks), jnp.bfloat16),
            dma((sp, 2)), dma((sp, 2)), dma((4,)), dma((chunks,)), dma((chunks,)),
        ],
        compiler_params=pltpu.CompilerParams(
            collective_id=1, has_side_effects=True, vmem_limit_bytes=ALL_VMEM
        ),
    )(stick, delta, sb_out_w, delta_out_w)
    return result.reshape(1, rows // tp, width)


def on_device(*inputs):
    delta_heads = inputs[11].shape[0]
    square = lax.axis_size("fs") == 4 and lax.axis_size("tp") == 2
    if square and delta_heads == lax.axis_size("sp") and inputs[4].shape[0] % delta_heads == 0:
        return on_device_heads(*inputs)
    return on_device_split(*inputs)


def solution(mesh):
    return jax.shard_map(
        on_device,
        mesh=mesh,
        in_specs=(
            P("fs", "sp", "tp"),
            P("fs", "tp"),
            P("fs", "tp"),
            P("fs", "tp"),
            P("tp"),
            P("fs", "tp"),
            P("fs", "tp"),
            P("fs", "tp"),
            P(None, "tp"),
            P(None, "tp"),
            P("tp"),
            P("tp"),
            P("fs", "tp", "sp"),
            P(),
            P("tp", None),
            P("tp", None),
        ),
        out_specs=P("fs", ("sp", "tp"), None),
        check_vma=False,
    )
```
